32 devices in a mesh: ep: 8 (over z, x), tp: 4 (over y, core).
Axes of the slice: x: 2, y: 2, z: 4, core: 2. Of those that a mesh axis runs over, the one named last changes fastest.
Arguments:
- queries: bfloat16 [2048, 2, 1024], P('ep', None, 'tp')
- keys: bfloat16 [2048, 2, 256], P('ep', None, 'tp')
- values: bfloat16 [2048, 2, 256], P('ep', None, 'tp'), may hold values from -6 to 6
- query_gain: float32 [64], replicated, may hold values from 1.2 to 6
- key_gain: float32 [64], replicated, may hold values from 1.2 to 6
- out_weight: bfloat16 [1024, 2048], P('tp'), may hold values from -0.75 to 0.75
- moe_tokens: bfloat16 [4096, 2048], P(('ep', 'tp')), may hold values from -6 to 6
- moe_gain: float32 [2048], replicated, may hold values from 0.1 to 1.9
- routes: int32 [4096, 2], P(('ep', 'tp')), may hold values from 0 to 7, all different within a row; in each aligned block of 128 rows (0 to 127, 128 to 255, ...) at most 48 rows name the same one
- route_weight: float32 [4096, 2], P(('ep', 'tp')), may hold values from 0.1 to 1
- w_gate: bfloat16 [8, 2048, 1024], P('ep', None, 'tp'), may hold values from -0.125 to 0.125
- w_up: bfloat16 [8, 2048, 1024], P('ep', None, 'tp'), may hold values from -0.125 to 0.125
- w_down: bfloat16 [8, 1024, 2048], P('ep', 'tp'), may hold values from -0.1875 to 0.1875
Outputs:
- attended: bfloat16 [2048, 2, 2048], P(('ep', 'tp'))
- routed: bfloat16 [4096, 2048], P(('ep', 'tp'))
The draws below stay inside these ranges and needn't reach their ends.
Inputs may be any that keep to these rules, and one draw needn't show every extreme that they name: `routes`: each row names 2 different experts. The rows of one device name no expert more than 48 times, and in every draw some device's rows name one expert exactly 48 times.
All inputs are finite; a program needn't handle non-finite values.
Results may differ from the reference program's by a relative error of at most 0.013.
The reference program's roundings to bfloat16 on the way count: a program that leaves them out, or rounds other values in their place, can miss the bound.
Values may be sent and summed in bfloat16 or wider, within the bound.
A program may use at most 128 MiB of HBM per device.

```python
import math
import jax
import jax.numpy as jnp
import numpy as np
from jax import lax

D = 2048
HEADS = 16
KV_HEADS = 4
HEAD_DIM = 64
FF = 1024
TOPK = 2
GRID_W = 64
SEQS = 2
TOK_DEV = 128
LEN = 2048
EXPERTS = 8
CAP = 48
TOKENS = 4096
N_EP = 8
N_TP = 4


def draw_both(key):
    keys_drawn = jax.random.normal(jax.random.fold_in(key, 12), (LEN, SEQS, KV_HEADS * HEAD_DIM), jnp.float32)
    queries_drawn = jax.random.normal(jax.random.fold_in(key, 11), (LEN, SEQS, HEADS * HEAD_DIM), jnp.float32)
    return (queries_drawn, keys_drawn)


def draw_queries(key, part):
    return draw_both(key)[0].astype(jnp.bfloat16)


def draw_keys(key, part):
    return draw_both(key)[1].astype(jnp.bfloat16)


def draw_gain_values(key):
    return jax.random.uniform(key, (HEAD_DIM,), jnp.float32, 1.2, 2.0)


def draw_query_gain(key, part):
    return draw_gain_values(jax.random.fold_in(key, 21))


def draw_key_gain(key, part):
    return draw_gain_values(jax.random.fold_in(key, 22))


def shard_levels(own_key, shape, split, least, high):
    def one(position, blocks):
        draws = jax.random.uniform(jax.random.fold_in(jax.random.fold_in(own_key, 6), position), (blocks,), jnp.float32, least / len(split), high / len(split))
        return jnp.repeat(jnp.exp(draws), shape[position] // blocks).reshape((-1,) + (1,) * (len(shape) - position - 1))

    level = one(*split[0])
    for cut in split[1:]:
        level = level * one(*cut)
    return level


def shared_out(key, own, number, rows, count, top, limit, skew):
    order = jax.random.permutation(key, count)
    heavy_load, common = load_shares(count, rows * top, limit, skew, True), load_shares(count, rows * top, limit, skew, False)
    places = jnp.arange(count)

    def named(sizes, turn):
        used = int((sizes > 0).sum())
        fixed = max(1, used // 4)
        passed = fixed + (places - fixed + turn * (used - fixed)) % max(1, count - fixed)
        return jnp.zeros((count,), jnp.int32).at[order[jnp.where(places < fixed, places, passed)]].set(jnp.asarray(sizes, jnp.int32))

    sizes = jnp.where(number % 4 == 0, named(heavy_load, number // 4), named(common, number - number // 4 - 1))
    mixed = jax.random.permutation(jax.random.fold_in(own, 3), count)
    source_of, sink = mixed[0:count // 2 * 2:2], mixed[1:count // 2 * 2:2]
    margin = jnp.minimum(sizes[source_of] - 1, limit - sizes[sink]) // 2
    margin = jnp.where((source_of == order[0]) | (sink == order[0]) | (sizes[sink] == 0), 0, jnp.maximum(margin, 0))
    passed = jax.random.randint(jax.random.fold_in(own, 4), (count // 2,), 0, 1 << 20) % (margin + 1)
    sizes = sizes.at[source_of].add(-passed).at[sink].add(passed)
    members = jnp.searchsorted(jnp.cumsum(sizes), jnp.arange(rows * top), side="right").astype(jnp.int32)
    table = members.reshape(top, rows).T
    table = table[jax.random.permutation(jax.random.fold_in(own, 1), rows)]
    turn = jax.random.randint(jax.random.fold_in(own, 2), (rows, 1), 0, top)
    return jnp.take_along_axis(table, (jnp.arange(top)[None, :] + turn) % top, axis=1)


def load_shares(number_of, total, most, slope, full):
    weights = [(1 << 20) // math.isqrt(standing ** slope) + 1 for standing in range(1, number_of + 1)]
    largest = most if full else min(most, max(-(-total // number_of), total * weights[0] // sum(weights)))
    least = 1 if total - largest >= number_of - 1 else 0
    counts, spare = [largest] + [least] * (number_of - 1), total - largest - least * (number_of - 1)
    while spare > 0:
        movable = [i for i in range(1, number_of) if counts[i] < largest] or [i for i in range(1, number_of) if counts[i] < most]
        whole, budget = sum([weights[i] for i in movable]), spare
        for i in movable:
            addition = min(most - counts[i], max(1, budget * weights[i] // whole), spare)
            counts[i] = counts[i] + addition
            spare = spare - addition
    return np.array(counts)


def normal_values(rng, shape, scale, limit, cuts=(), held_as=jnp.bfloat16):
    result = scale * jax.random.normal(rng, shape, jnp.float32)
    if cuts:
        result = result * shard_levels(rng, shape, cuts, -0.22, 0.18)
    return jnp.clip(result, -limit, limit).astype(held_as)


def setup_inputs(seed: int = 0) -> dict:
    seeds = jax.random.split(jax.random.key(seed), 14)
    queries = draw_queries(jax.random.fold_in(seeds[13], 71), 0)
    keys = draw_keys(jax.random.fold_in(seeds[13], 71), 0)
    values = normal_values(seeds[2], (LEN, SEQS, KV_HEADS * HEAD_DIM), 1.0, 6.0, ((0, 8), (2, 4)))
    query_gain = draw_query_gain(jax.random.fold_in(seeds[13], 71), 0)
    key_gain = draw_key_gain(jax.random.fold_in(seeds[13], 71), 0)
    out_weight = normal_values(seeds[5], (HEADS * HEAD_DIM, D), (HEADS * HEAD_DIM // 16) ** -0.5, 0.75, ((0, 4),))
    moe_tokens = normal_values(seeds[6], (TOKENS, D), 1.0, 6.0, ((0, 32),))
    moe_gain = jnp.clip(1.0 + 0.18 * jax.random.normal(seeds[7], (D,), jnp.float32), 0.1, 1.9)
    routes_keys = jax.random.split(jax.random.fold_in(seeds[8], 1), TOKENS // TOK_DEV)
    routes_turns = jax.random.permutation(jax.random.fold_in(seeds[8], 3), TOKENS // TOK_DEV)
    routes = jax.vmap(lambda own, number: shared_out(jax.random.fold_in(seeds[8], 2), own, number, TOK_DEV, EXPERTS, TOPK, CAP, 1))(routes_keys, routes_turns).reshape((TOKENS, TOPK))
    route_weight = jnp.clip(0.1 + 0.9 * jax.random.uniform(seeds[9], (TOKENS, TOPK), jnp.float32) ** shard_levels(seeds[9], (TOKENS, TOPK), ((0, 32),), -0.2, 0.2), 0.1, 1.0)
    w_gate = normal_values(seeds[10], (EXPERTS, D, FF), D ** -0.5, 0.125, ((0, 8), (2, 4)))
    w_up = normal_values(seeds[11], (EXPERTS, D, FF), D ** -0.5, 0.125, ((0, 8), (2, 4)))
    w_down = normal_values(seeds[12], (EXPERTS, FF, D), FF ** -0.5, 0.1875, ((0, 8), (1, 4)))
    return dict(queries=queries, keys=keys, values=values, query_gain=query_gain, key_gain=key_gain, out_weight=out_weight, moe_tokens=moe_tokens, moe_gain=moe_gain, routes=routes, route_weight=route_weight, w_gate=w_gate, w_up=w_up, w_down=w_down)


EPS = 1e-06
THETA = 10000.0

def turn(normed, positions):
    quarter = normed.shape[-1] // 4
    inverse = THETA ** (-jnp.arange(quarter, dtype=jnp.float32) / quarter)
    grid_row = (positions // GRID_W).astype(jnp.float32)
    grid_col = (positions % GRID_W).astype(jnp.float32)
    angles = jnp.stack([grid_row[:, None] * inverse, grid_col[:, None] * inverse], axis=1)
    cosine = jnp.cos(angles)[:, None, None]
    sine = jnp.sin(angles)[:, None, None]
    parts = normed.reshape(normed.shape[:-1] + (2, 2, quarter))
    first = parts[..., 0, :]
    second = parts[..., 1, :]
    turned = jnp.stack([first * cosine - second * sine, second * cosine + first * sine], axis=-2)
    return turned.reshape(normed.shape)

def prepare(data, positions, gain):
    heads = data.astype(jnp.float32).reshape(data.shape[0], data.shape[1], -1, HEAD_DIM)
    normed = heads * lax.rsqrt(lax.optimization_barrier(jnp.mean(heads * heads, axis=-1, keepdims=True)) + EPS) * gain
    return turn(normed, positions).astype(jnp.bfloat16)

def reference(queries, keys, values, query_gain, key_gain, out_weight, moe_tokens, moe_gain, routes, route_weight, w_gate, w_up, w_down):
    positions = jnp.arange(LEN, dtype=jnp.int32)
    q_rot = prepare(queries, positions, query_gain)
    k_rot = prepare(keys, positions, key_gain)
    key_float = k_rot.astype(jnp.float32)
    value_float = values.reshape(LEN, SEQS, KV_HEADS, HEAD_DIM).astype(jnp.float32)
    groups = HEADS // KV_HEADS
    block = math.gcd(LEN, 64)
    query_blocks = q_rot.reshape(LEN // block, block, SEQS, KV_HEADS, groups, HEAD_DIM)

    def attend(query_block):
        scores = jnp.einsum('bskgd,lskd->skgbl', query_block.astype(jnp.float32), key_float) * HEAD_DIM ** (-0.5)
        largest = lax.optimization_barrier(jnp.max(scores, axis=-1, keepdims=True))
        expo = jnp.exp(scores - largest)
        total = lax.optimization_barrier(jnp.sum(expo, axis=-1))
        probs = lax.optimization_barrier(expo.astype(jnp.bfloat16)).astype(jnp.float32)
        summed = jnp.einsum('skgbl,lskd->skgbd', probs, value_float) / total[..., None]
        return jnp.transpose(summed, (3, 0, 1, 2, 4)).astype(jnp.bfloat16)
    mixed = lax.map(attend, query_blocks).reshape(LEN * SEQS, HEADS * HEAD_DIM)
    width = HEADS * HEAD_DIM // N_TP
    accum = jnp.zeros((LEN * SEQS, D), jnp.float32)
    for index in range(N_TP):
        part = jnp.dot(mixed[:, index * width:(index + 1) * width], out_weight[index * width:(index + 1) * width], preferred_element_type=jnp.float32)
        accum = accum + lax.optimization_barrier(part.astype(jnp.bfloat16)).astype(jnp.float32)
    attended = accum.astype(jnp.bfloat16).reshape(LEN, SEQS, D)
    token_float = moe_tokens.astype(jnp.float32)
    normed = (token_float * lax.rsqrt(lax.optimization_barrier(jnp.mean(token_float * token_float, axis=-1, keepdims=True)) + EPS) * moe_gain).astype(jnp.bfloat16)
    most = N_EP * N_TP * CAP
    unit_width = FF // N_TP

    def expert(carry, item):
        index, gate_weight, up_weight, down_weight = item
        chosen = routes == index
        weight = lax.optimization_barrier(jnp.sum(jnp.where(chosen, route_weight, 0.0), axis=1))
        live = jnp.any(chosen, axis=1)
        rows = jnp.nonzero(live, size=most, fill_value=0)[0].astype(jnp.int32)
        count = jnp.sum(live.astype(jnp.int32))
        valid = (jnp.arange(most, dtype=jnp.int32) < count).astype(jnp.float32)
        picked = normed[rows]
        gate = jnp.dot(picked, gate_weight, preferred_element_type=jnp.float32)
        up = jnp.dot(picked, up_weight, preferred_element_type=jnp.float32)
        hidden = (jax.nn.silu(gate) * up).astype(jnp.bfloat16)
        out = jnp.zeros((most, D), jnp.float32)
        for block_index in range(N_TP):
            part = jnp.dot(hidden[:, block_index * unit_width:(block_index + 1) * unit_width], down_weight[block_index * unit_width:(block_index + 1) * unit_width], preferred_element_type=jnp.float32)
            out = out + lax.optimization_barrier(part.astype(jnp.bfloat16)).astype(jnp.float32)
        expert_out = lax.optimization_barrier(out.astype(jnp.bfloat16)).astype(jnp.float32)
        contrib = expert_out * (weight[rows] * valid)[:, None]
        return (carry.at[rows].add(contrib), None)
    routed, _ = lax.scan(expert, jnp.zeros((TOKENS, D), jnp.float32), (jnp.arange(EXPERTS, dtype=jnp.int32), w_gate, w_up, w_down))
    return (attended, routed.astype(jnp.bfloat16))
```

```python
import functools
import math

import jax
import jax.numpy as jnp
from jax import lax
from jax.experimental import pallas as pl
from jax.experimental.pallas import tpu as pltpu
from jax.sharding import PartitionSpec as P

HEAD_DIM = 64
GRID_W = 64


EPS = 1e-06
THETA = 10000.0


def turn(normed, positions):
    quarter = normed.shape[-1] // 4
    inverse = THETA ** (-jnp.arange(quarter, dtype=jnp.float32) / quarter)
    grid_row = (positions // GRID_W).astype(jnp.float32)
    grid_col = (positions % GRID_W).astype(jnp.float32)
    angles = jnp.stack([grid_row[:, None] * inverse, grid_col[:, None] * inverse], axis=1)
    cosine = jnp.cos(angles)[:, None, None]
    sine = jnp.sin(angles)[:, None, None]
    parts = normed.reshape(normed.shape[:-1] + (2, 2, quarter))
    first = parts[..., 0, :]
    second = parts[..., 1, :]
    turned = jnp.stack([first * cosine - second * sine, second * cosine + first * sine], axis=-2)
    return turned.reshape(normed.shape)


def prepare(data, positions, gain):
    heads = data.astype(jnp.float32).reshape(data.shape[0], data.shape[1], -1, HEAD_DIM)
    normed = heads * lax.rsqrt(jnp.mean(heads * heads, axis=-1, keepdims=True) + EPS) * gain
    return turn(normed, positions).astype(jnp.bfloat16)


MESH = pl.DeviceIdType.MESH


def greet(partners):
    barrier = pltpu.get_barrier_semaphore()
    for device in partners:
        pl.semaphore_signal(barrier, inc=1, device_id=device, device_id_type=MESH)
    pl.semaphore_wait(barrier, len(partners))


def all_partners(e, t, experts):
    low, high = t + 1 - 2 * (t % 2), (t + 2) % 4
    return low, high, [((e + k) % experts, t) for k in range(1, experts)] + [(e, low), (e, high)]


def dispatch_kernel(experts, send, kv, out, kv_out, *sems):
    e, t = lax.axis_index("ep"), lax.axis_index("tp")
    low, high, partners = all_partners(e, t, experts)
    (a_send, a_recv, y_send, y_recv, l_send, l_recv, m_send, m_recv, k_send, k_recv, x_send, x_recv, own) = sems
    half = experts // 2
    side = e + 1 - 2 * (e % 2)

    def remote(src, dst, s, r, device):
        return pltpu.make_async_remote_copy(
            src_ref=src, dst_ref=dst, send_sem=s, recv_sem=r, device_id=device, device_id_type=MESH
        )

    def kv_direct(k):
        return remote(kv, kv_out.at[e], k_send.at[k], k_recv.at[k], ((e + 2 * k) % experts, t))

    def kv_side(k):
        owner = (e - 2 * k + experts) % experts
        return remote(kv_out.at[owner], kv_out.at[owner], x_send.at[k], x_recv.at[k], (side, t))

    def chunk(k):
        return remote(send.at[(e + k) % experts], out.at[t, e], a_send.at[k], a_recv.at[k], ((e + k) % experts, t))

    def source(k):
        return (e - k + experts) % experts

    def across(k):
        block = out.at[t, source(k)]
        return remote(block, block, y_send.at[k], y_recv.at[k], (e, high))

    def beside(k):
        block = out.at[t, source(k)]
        return remote(block, block, l_send.at[k], l_recv.at[k], (e, low))

    def relay(k):
        block = out.at[high, source(k)]
        return remote(block, block, m_send.at[k], m_recv.at[k], (e, low))

    greet(partners)
    own_chunk = pltpu.make_async_copy(send.at[e], out.at[t, e], own.at[0])
    own_chunk.start()
    own_kv = pltpu.make_async_copy(kv, kv_out.at[e], own.at[1])
    own_kv.start()
    lax.fori_loop(1, half, lambda k, c: (kv_direct(k).start(), c)[1], 0)
    lax.fori_loop(1, experts, lambda k, c: (chunk(k).start(), c)[1], 0)
    own_chunk.wait()
    own_kv.wait()
    across(0).start()
    beside(0).start()
    kv_side(0).start()

    def step(k, carry):
        chunk(k).wait_recv()
        across(k).start()
        beside(k).start()

        @pl.when(k < half)
        def _():
            kv_direct(k).wait_recv()
            kv_side(k).start()

        @pl.when(k >= 2)
        def _():
            across(k - 2).wait_recv()
            relay(k - 2).start()

        return carry

    lax.fori_loop(1, experts, step, 0)
    for k in range(experts - 2, experts):
        across(k).wait_recv()
        relay(k).start()

    def finish(k, carry):
        across(k).wait_send()
        beside(k).wait()
        relay(k).wait()

        @pl.when(k >= 1)
        def _():
            chunk(k).wait_send()

        @pl.when(k < half)
        def _():
            kv_side(k).wait()

        @pl.when((k >= 1) & (k < half))
        def _():
            kv_direct(k).wait_send()

        return carry

    lax.fori_loop(0, experts, finish, 0)


def exchange(experts, send, kv):
    vmem = pl.BlockSpec(memory_space=pltpu.VMEM)
    sem = pltpu.SemaphoreType.DMA((experts,))
    return pl.pallas_call(
        functools.partial(dispatch_kernel, experts),
        out_shape=(
            jax.ShapeDtypeStruct((4,) + send.shape, send.dtype),
            jax.ShapeDtypeStruct((experts,) + kv.shape, kv.dtype),
        ),
        in_specs=[vmem, vmem],
        out_specs=(vmem, vmem),
        scratch_shapes=[sem] * 12 + [pltpu.SemaphoreType.DMA((2,))],
        name="dispatch",
        compiler_params=pltpu.CompilerParams(
            collective_id=1, has_side_effects=True, vmem_limit_bytes=58 * 2**20
        ),
    )(send, kv)


def collect_kernel(experts, part, prod, ret, att, pair, pair_att, gone, gone_att, seen, seen_att, done, *sems):
    e, t = lax.axis_index("ep"), lax.axis_index("tp")
    low, high, partners = all_partners(e, t, experts)
    low_high = (low + 2) % 4
    (p_send, p_recv, q_send, q_recv, y_send, y_recv, a_send, a_recv, o_send, o_recv, own) = sems
    middle = experts // 2

    def remote(src, dst, s, r, device):
        return pltpu.make_async_remote_copy(
            src_ref=src, dst_ref=dst, send_sem=s, recv_sem=r, device_id=device, device_id_type=MESH
        )

    def target(k):
        return (e + middle + k) % experts

    def pair_far(k):
        return remote(part.at[low_high, target(k)], pair.at[1, k], p_send.at[k], p_recv.at[k], (e, low))

    def pair_near(k):
        return remote(part.at[low, target(k)], pair.at[0, k], q_send.at[k], q_recv.at[k], (e, low))

    def across(k):
        return remote(gone.at[k], seen.at[k], y_send.at[k], y_recv.at[k], (e, high))

    def back(k):
        return remote(done.at[k], ret.at[e], a_send.at[k], a_recv.at[k], (target(k), t))

    def other(i):
        if i < 2:
            return remote(prod.at[(low, low_high)[i]], pair_att.at[i], o_send.at[i], o_recv.at[i], (e, low))
        return remote(gone_att, seen_att, o_send.at[i], o_recv.at[i], (e, high))

    def local():
        return pltpu.make_async_copy(done.at[middle], ret.at[e], own.at[0])

    def deliver(k):
        @pl.when(k == middle)
        def _():
            local().start()

        @pl.when(k != middle)
        def _():
            back(k).start()

    f32 = jnp.float32
    greet(partners)
    lax.fori_loop(0, experts, lambda k, c: (pair_far(k).start(), c)[1], 0)
    other(1).start()
    lax.fori_loop(0, experts, lambda k, c: (pair_near(k).start(), c)[1], 0)
    other(0).start()

    def first(k, carry):
        pair_far(k).wait_recv()
        gone[k] = (part[high, target(k)].astype(f32) + pair[1, k].astype(f32)).astype(gone.dtype)

        @pl.when(k >= 1)
        def _():
            across(k - 1).start()

        return carry

    lax.fori_loop(0, experts, first, 0)
    other(1).wait_recv()
    gone_att[...] = (prod[high].astype(f32) + pair_att[1].astype(f32)).astype(gone_att.dtype)
    across(experts - 1).start()

    def second(k, carry):
        pair_near(k).wait_recv()
        across(k).wait_recv()

        @pl.when(k == 0)
        def _():
            other(2).start()

        total = part[t, target(k)].astype(f32) + pair[0, k].astype(f32) + seen[k].astype(f32)
        done[k] = total.astype(done.dtype)

        @pl.when(k >= 1)
        def _():
            deliver(k - 1)

        return carry

    lax.fori_loop(0, experts, second, 0)
    other(0).wait_recv()
    deliver(experts - 1)
    other(2).wait_recv()
    att[...] = (prod[t].astype(f32) + pair_att[0].astype(f32) + seen_att[...].astype(f32)).astype(att.dtype)

    def finish(k, carry):
        pair_far(k).wait_send()
        pair_near(k).wait_send()
        across(k).wait_send()

        @pl.when(k == middle)
        def _():
            local().wait()

        @pl.when(k != middle)
        def _():
            back(k).wait()

        return carry

    lax.fori_loop(0, experts, finish, 0)
    for i in range(3):
        other(i).wait_send()


def collect(experts, part, prod):
    vmem = pl.BlockSpec(memory_space=pltpu.VMEM)
    sem = pltpu.SemaphoreType.DMA((experts,))
    row, att = part.shape[1:], prod.shape[1:]
    like = part.dtype
    return pl.pallas_call(
        functools.partial(collect_kernel, experts),
        out_shape=(jax.ShapeDtypeStruct(row, like), jax.ShapeDtypeStruct(att, like)),
        in_specs=[vmem, vmem],
        out_specs=(vmem, vmem),
        scratch_shapes=[
            pltpu.VMEM((2,) + row, like),
            pltpu.VMEM((2,) + att, like),
            pltpu.VMEM(row, like),
            pltpu.VMEM(att, like),
            pltpu.VMEM(row, like),
            pltpu.VMEM(att, like),
            pltpu.VMEM(row, like),
        ]
        + [sem] * 8
        + [pltpu.SemaphoreType.DMA((3,))] * 2
        + [pltpu.SemaphoreType.DMA((1,))],
        name="collect",
        compiler_params=pltpu.CompilerParams(
            collective_id=2, has_side_effects=True, vmem_limit_bytes=58 * 2**20
        ),
    )(part, prod)


def per_device(
    queries,
    keys,
    values,
    query_gain,
    key_gain,
    out_weight,
    moe_tokens,
    moe_gain,
    routes,
    route_weight,
    w_gate,
    w_up,
    w_down,
):
    pos_count = queries.shape[0]
    seq_count = queries.shape[1]
    positions = lax.axis_index("ep") * pos_count + jnp.arange(pos_count, dtype=jnp.int32)
    q_rot = prepare(queries, positions, query_gain)
    k_rot = prepare(keys, positions, key_gain)
    kv_local = k_rot.shape[2]
    groups = q_rot.shape[2] // kv_local
    value_heads = values.reshape(pos_count, seq_count, kv_local, HEAD_DIM)
    q_group = q_rot.reshape(pos_count, seq_count, kv_local, groups, HEAD_DIM)
    scale = HEAD_DIM ** (-0.5)
    tok_count = moe_tokens.shape[0]
    top_count = routes.shape[1]
    experts = lax.axis_size("ep")
    capacity = max(2, (3 * tok_count * top_count + 2 * experts - 1) // (2 * experts))
    token_float = moe_tokens.astype(jnp.float32)
    normed = (
        token_float
        * lax.rsqrt(jnp.mean(token_float * token_float, axis=-1, keepdims=True) + EPS)
        * moe_gain
    ).astype(jnp.bfloat16)
    hits = (routes[:, :, None] == jnp.arange(experts, dtype=jnp.int32)[None, None, :]).astype(
        jnp.float32
    )
    pair_count = tok_count * top_count
    flat_hits = hits.reshape(pair_count, experts)
    pair_index = jnp.arange(pair_count, dtype=jnp.int32)
    earlier = (pair_index[:, None] > pair_index[None, :]).astype(jnp.float32)
    before = jnp.dot(earlier, flat_hits, precision=lax.Precision.HIGHEST)
    rank = jnp.sum(before * flat_hits, axis=-1).astype(jnp.int32).reshape(tok_count, top_count)
    slot = routes * capacity + rank
    table = jnp.arange(experts * capacity, dtype=jnp.int32)
    dispatch = jnp.sum(
        (slot[None, :, :] == table[:, None, None]).astype(jnp.float32), axis=2
    ).astype(jnp.bfloat16)
    send = jnp.dot(dispatch, normed, preferred_element_type=jnp.float32).astype(jnp.bfloat16)
    start_state = (
        jnp.full((seq_count, kv_local, groups, pos_count), -1e30, jnp.float32),
        jnp.zeros((seq_count, kv_local, groups, pos_count), jnp.float32),
        jnp.zeros((pos_count, seq_count, kv_local, groups, HEAD_DIM), jnp.float32),
    )
    carry = start_state
    kv = jnp.concatenate([k_rot, value_heads], axis=-1)
    kv = jnp.transpose(kv, (1, 2, 0, 3)).reshape(seq_count * kv_local * pos_count, 2 * HEAD_DIM)
    rows, kv_all = exchange(experts, send.reshape(experts, capacity, -1), kv)
    kv_all = kv_all.reshape(experts, seq_count, kv_local, pos_count, 2 * HEAD_DIM)
    kv_all = jnp.transpose(kv_all, (0, 3, 1, 2, 4)).reshape(experts * pos_count, seq_count, kv_local, 2 * HEAD_DIM)
    key_piece = kv_all[..., :HEAD_DIM]
    value_piece = kv_all[..., HEAD_DIM:]
    count = key_piece.shape[0]
    width = math.gcd(count, 512)
    key_split = key_piece.reshape(count // width, width, seq_count, kv_local, HEAD_DIM)
    value_split = value_piece.reshape(count // width, width, seq_count, kv_local, HEAD_DIM)

    def step(state, block):
        best, total, accum = state
        key_block, value_block = block
        scores = (
            jnp.einsum("pskgd,lskd->skgpl", q_group, key_block, preferred_element_type=jnp.float32)
            * scale
        )
        new_best = jnp.maximum(best, jnp.max(scores, axis=-1))
        factor = jnp.exp(best - new_best)
        expo = jnp.exp(scores - new_best[..., None])
        total = total * factor + jnp.sum(expo, axis=-1)
        added = jnp.einsum(
            "skgpl,lskd->pskgd",
            expo.astype(jnp.bfloat16),
            value_block,
            preferred_element_type=jnp.float32,
        )
        accum = accum * jnp.transpose(factor, (3, 0, 1, 2))[..., None] + added
        return ((new_best, total, accum), None)

    carry, _ = lax.scan(step, carry, (key_split, value_split))
    best, total, accum = carry
    mixed = (accum / jnp.transpose(total, (3, 0, 1, 2))[..., None]).astype(jnp.bfloat16)
    mixed = mixed.reshape(pos_count, seq_count, -1)
    product = jnp.dot(
        mixed.reshape(pos_count * seq_count, -1),
        out_weight,
        preferred_element_type=jnp.float32,
    )
    tp = lax.axis_size("tp")
    gathered = rows.reshape(tp * experts * capacity, -1)
    gate = jnp.dot(gathered, w_gate[0], preferred_element_type=jnp.float32)
    up = jnp.dot(gathered, w_up[0], preferred_element_type=jnp.float32)
    hidden = (jax.nn.silu(gate) * up).astype(jnp.bfloat16)
    part = jnp.dot(hidden, w_down[0], preferred_element_type=jnp.float32).astype(jnp.bfloat16)
    returned_rows, attended = collect(
        experts,
        part.reshape(tp, experts, capacity, -1),
        product.astype(jnp.bfloat16).reshape(tp, pos_count // tp * seq_count, -1),
    )
    returned_rows = returned_rows.reshape(experts * capacity, -1)
    attended = attended.reshape(pos_count // tp, seq_count, -1)
    combined = jnp.zeros((tok_count, returned_rows.shape[-1]), jnp.float32)
    for choice_index in range(top_count):
        picker = (slot[:, choice_index : choice_index + 1] == table[None, :]).astype(jnp.bfloat16)
        picked = jnp.dot(picker, returned_rows, preferred_element_type=jnp.float32)
        combined = combined + picked * route_weight[:, choice_index : choice_index + 1]
    return (attended, combined.astype(jnp.bfloat16))


def solution(mesh):
    in_specs = (
        P("ep", None, "tp"),
        P("ep", None, "tp"),
        P("ep", None, "tp"),
        P(),
        P(),
        P("tp", None),
        P(("ep", "tp"), None),
        P(),
        P(("ep", "tp"), None),
        P(("ep", "tp"), None),
        P("ep", None, "tp"),
        P("ep", None, "tp"),
        P("ep", "tp", None),
    )
    out_specs = (P(("ep", "tp"), None, None), P(("ep", "tp"), None))
    return jax.shard_map(
        per_device, mesh=mesh, in_specs=in_specs, out_specs=out_specs, check_vma=False
    )
```

```python
import functools

import jax
import jax.numpy as jnp
from jax import lax
from jax.experimental import pallas as pl
from jax.experimental.pallas import tpu as pltpu
from jax.sharding import PartitionSpec as P

HEAD_DIM = 64
GRID_W = 64


EPS = 1e-06
THETA = 10000.0


def turn(normed, positions):
    quarter = normed.shape[-1] // 4
    inverse = THETA ** (-jnp.arange(quarter, dtype=jnp.float32) / quarter)
    grid_row = (positions // GRID_W).astype(jnp.float32)
    grid_col = (positions % GRID_W).astype(jnp.float32)
    angles = jnp.stack([grid_row[:, None] * inverse, grid_col[:, None] * inverse], axis=1)
    cosine = jnp.cos(angles)[:, None, None]
    sine = jnp.sin(angles)[:, None, None]
    parts = normed.reshape(normed.shape[:-1] + (2, 2, quarter))
    first = parts[..., 0, :]
    second = parts[..., 1, :]
    turned = jnp.stack([first * cosine - second * sine, second * cosine + first * sine], axis=-2)
    return turned.reshape(normed.shape)


def prepare(data, positions, gain):
    heads = data.astype(jnp.float32).reshape(data.shape[0], data.shape[1], -1, HEAD_DIM)
    normed = heads * lax.rsqrt(jnp.mean(heads * heads, axis=-1, keepdims=True) + EPS) * gain
    return turn(normed, positions).astype(jnp.bfloat16)


MESH = pl.DeviceIdType.MESH


def fused_kernel(experts, send, kv, q, out_weight, w_gate, w_up, w_down, ret, att, *scratch):
    (rows, kv_all, part, pair, gone, seen, done, prod, pair_att, gone_att, seen_att, packed, accum, best, total) = scratch[:15]
    (a_send, a_recv, y_send, y_recv, l_send, l_recv, m_send, m_recv, k_send, k_recv, x_send, x_recv) = scratch[15:27]
    (f_send, f_recv, n_send, n_recv, c_send, c_recv, b_send, b_recv, o_send, o_recv, own) = scratch[27:]
    f32, bf16 = jnp.float32, jnp.bfloat16
    e, t = lax.axis_index("ep"), lax.axis_index("tp")
    low, high = t + 1 - 2 * (t % 2), (t + 2) % 4
    low_high = (low + 2) % 4
    half = experts // 2
    side = e + 1 - 2 * (e % 2)
    capacity = send.shape[1]
    stride = packed.shape[0] // 4

    def remote(src, dst, s, r, device):
        return pltpu.make_async_remote_copy(
            src_ref=src, dst_ref=dst, send_sem=s, recv_sem=r, device_id=device, device_id_type=MESH
        )

    def source(k):
        return (e - k + experts) % experts

    def kv_direct(k):
        return remote(kv, kv_all.at[e], k_send.at[k], k_recv.at[k], ((e + 2 * k) % experts, t))

    def kv_side(k):
        block = kv_all.at[(e - 2 * k + experts) % experts]
        return remote(block, block, x_send.at[k], x_recv.at[k], (side, t))

    def chunk(k):
        return remote(send.at[(e + k) % experts], rows.at[t, e], a_send.at[k], a_recv.at[k], ((e + k) % experts, t))

    def across(k):
        block = rows.at[t, source(k)]
        return remote(block, block, y_send.at[k], y_recv.at[k], (e, high))

    def beside(k):
        block = rows.at[t, source(k)]
        return remote(block, block, l_send.at[k], l_recv.at[k], (e, low))

    def relay(k):
        block = rows.at[high, source(k)]
        return remote(block, block, m_send.at[k], m_recv.at[k], (e, low))

    def pair_far(k):
        return remote(part.at[low_high, k], pair.at[1, k], f_send.at[k], f_recv.at[k], (e, low))

    def pair_near(k):
        return remote(part.at[low, k], pair.at[0, k], n_send.at[k], n_recv.at[k], (e, low))

    def over(k):
        return remote(gone.at[k], seen.at[k], c_send.at[k], c_recv.at[k], (e, high))

    def back(k):
        return remote(done.at[k], ret.at[e], b_send.at[k], b_recv.at[k], (source(k), t))

    def other(i):
        if i < 2:
            return remote(prod.at[(low, low_high)[i]], pair_att.at[i], o_send.at[i], o_recv.at[i], (e, low))
        return remote(gone_att, seen_att, o_send.at[i], o_recv.at[i], (e, high))

    def attend(owner):
        for s in range(kv.shape[0]):
            block = kv_all[owner, s]
            scores = lax.dot_general(block, q[s], (((1,), (1,)), ((), ())), preferred_element_type=f32)
            old = best[s]
            new = jnp.maximum(old, jnp.max(scores, axis=0, keepdims=True))
            factor = jnp.exp(old - new)
            expo = jnp.exp(scores - new)
            best[s] = new
            total[s] = total[s] * factor + jnp.sum(expo, axis=0, keepdims=True)
            added = lax.dot_general(block, expo.astype(bf16), (((0,), (0,)), ((), ())), preferred_element_type=f32)
            accum[s] = accum[s] * factor + added

    def project():
        positions = kv.shape[1]
        quarter = positions // 4
        for s in range(kv.shape[0]):
            mixed = (accum[s, HEAD_DIM:, :] / total[s]).astype(bf16)
            groups = mixed.shape[1] // positions
            stacked = jnp.concatenate([mixed[:, g * positions : (g + 1) * positions] for g in range(groups)], axis=0)
            product = lax.dot_general(stacked, out_weight[...], (((0,), (0,)), ((), ())), preferred_element_type=f32)
            product = product.astype(bf16)
            for b in range(4):
                prod[b, s * quarter : (s + 1) * quarter, :] = product[b * quarter : (b + 1) * quarter]

    def expert(k):
        for b in range(4):
            packed[b * stride : b * stride + capacity, :] = rows[b, source(k)]
        data = packed[...]
        gate = jnp.dot(data, w_gate[...], preferred_element_type=f32)
        up = jnp.dot(data, w_up[...], preferred_element_type=f32)
        hidden = (gate * (1.0 / (1.0 + jnp.exp(-gate))) * up).astype(bf16)
        result = jnp.dot(hidden, w_down[...], preferred_element_type=f32).astype(bf16)
        for b in range(4):
            part[b, k] = result[b * stride : b * stride + capacity]

    barrier = pltpu.get_barrier_semaphore()
    partners = [((e + k) % experts, t) for k in range(1, experts)] + [(e, low), (e, high)]
    for device in partners:
        pl.semaphore_signal(barrier, inc=1, device_id=device, device_id_type=MESH)
    pl.semaphore_wait(barrier, len(partners))

    own_chunk = pltpu.make_async_copy(send.at[e], rows.at[t, e], own.at[0])
    own_chunk.start()
    own_kv = pltpu.make_async_copy(kv, kv_all.at[e], own.at[1])
    own_kv.start()
    lax.fori_loop(1, half, lambda k, c: (kv_direct(k).start(), c)[1], 0)
    lax.fori_loop(1, experts, lambda k, c: (chunk(k).start(), c)[1], 0)
    best[...] = jnp.full_like(best, -1e30)
    total[...] = jnp.zeros_like(total)
    accum[...] = jnp.zeros_like(accum)
    own_chunk.wait()
    own_kv.wait()
    kv_side(0).start()

    def step(k, carry):
        @pl.when((k >= 1) & (k < experts))
        def _():
            chunk(k).wait_recv()

        @pl.when(k < experts)
        def _():
            across(k).start()
            beside(k).start()

        @pl.when((k >= 1) & (k < half))
        def _():
            kv_direct(k).wait_recv()
            kv_side(k).start()

        @pl.when((k >= half) & (k < experts))
        def _():
            kv_side(k - half).wait_recv()

        @pl.when(k < experts)
        def _():
            direct = (e - 2 * k + 2 * experts) % experts
            beyond = (side - 2 * (k - half) + 2 * experts) % experts
            near = (experts + half - 1 - k) // experts
            attend(near * direct + (1 - near) * beyond)

        @pl.when(k == experts)
        def _():
            project()

        @pl.when(k == experts + 1)
        def _():
            other(1).start()
            other(0).start()

        @pl.when((k >= 2) & (k < experts + 2))
        def _():
            across(k - 2).wait_recv()
            relay(k - 2).start()

        @pl.when((k >= 4) & (k < experts + 4))
        def _():
            pair_far(k - 4).start()
            pair_near(k - 4).start()

        @pl.when((k >= 3) & (k < experts + 3))
        def _():
            beside(k - 3).wait_recv()
            relay(k - 3).wait_recv()
            expert(k - 3)

        @pl.when((k >= 6) & (k < experts + 6))
        def _():
            over(k - 6).start()

        @pl.when((k >= 5) & (k < experts + 5))
        def _():
            j = k - 5
            pair_far(j).wait_recv()
            gone[j] = (part[high, j].astype(f32) + pair[1, j].astype(f32)).astype(bf16)

        @pl.when(k == experts + 6)
        def _():
            other(1).wait_recv()
            gone_att[...] = (prod[high].astype(f32) + pair_att[1].astype(f32)).astype(bf16)

        @pl.when(k == experts + 7)
        def _():
            other(2).start()

        @pl.when(k == 9)
        def _():
            pltpu.make_async_copy(done.at[0], ret.at[e], own.at[0]).start()

        @pl.when((k >= 10) & (k < experts + 9))
        def _():
            back(k - 9).start()

        @pl.when((k >= 8) & (k < experts + 8))
        def _():
            j = k - 8
            pair_near(j).wait_recv()
            over(j).wait_recv()
            done[j] = (part[t, j].astype(f32) + pair[0, j].astype(f32) + seen[j].astype(f32)).astype(bf16)

        return carry

    lax.fori_loop(0, experts + 9, step, 0)
    other(0).wait_recv()
    other(2).wait_recv()
    att[...] = (prod[t].astype(f32) + pair_att[0].astype(f32) + seen_att[...].astype(f32)).astype(bf16)

    def finish(k, carry):
        across(k).wait_send()
        beside(k).wait_send()
        relay(k).wait_send()
        pair_far(k).wait_send()
        pair_near(k).wait_send()
        over(k).wait_send()

        @pl.when(k >= 1)
        def _():
            chunk(k).wait_send()
            back(k).wait()

        @pl.when(k < half)
        def _():
            kv_side(k).wait_send()

        @pl.when((k >= 1) & (k < half))
        def _():
            kv_direct(k).wait_send()

        return carry

    lax.fori_loop(0, experts, finish, 0)
    for i in range(3):
        other(i).wait_send()
    pltpu.make_async_copy(done.at[0], ret.at[e], own.at[0]).wait()


def fused(experts, send, kv, q, out_weight, w_gate, w_up, w_down):
    sem = pltpu.SemaphoreType.DMA((experts,))
    like = send.dtype
    capacity, features = send.shape[1:]
    seqs, positions, lanes = kv.shape
    att = (positions // 4 * seqs, features)
    queries = q.shape[1]
    stride = -(-capacity // 16) * 16
    shapes = [
        (4,) + send.shape,
        (experts,) + kv.shape,
        (4,) + send.shape,
        (2,) + send.shape,
        send.shape,
        send.shape,
        send.shape,
        (4,) + att,
        (2,) + att,
        att,
        att,
        (4 * stride, features),
    ]
    vmem = pl.BlockSpec(memory_space=pltpu.VMEM)
    return pl.pallas_call(
        functools.partial(fused_kernel, experts),
        out_shape=(jax.ShapeDtypeStruct(send.shape, like), jax.ShapeDtypeStruct(att, like)),
        in_specs=[vmem] * 7,
        out_specs=(vmem, vmem),
        scratch_shapes=[pltpu.VMEM(shape, like) for shape in shapes]
        + [
            pltpu.VMEM((seqs, lanes, queries), jnp.float32),
            pltpu.VMEM((seqs, 1, queries), jnp.float32),
            pltpu.VMEM((seqs, 1, queries), jnp.float32),
        ]
        + [sem] * 20
        + [pltpu.SemaphoreType.DMA((3,))] * 2
        + [pltpu.SemaphoreType.DMA((2,))],
        name="fused",
        compiler_params=pltpu.CompilerParams(
            collective_id=1, has_side_effects=True, vmem_limit_bytes=62 * 2**20
        ),
    )(send, kv, q, out_weight, w_gate, w_up, w_down)


def per_device(
    queries,
    keys,
    values,
    query_gain,
    key_gain,
    out_weight,
    moe_tokens,
    moe_gain,
    routes,
    route_weight,
    w_gate,
    w_up,
    w_down,
):
    pos_count = queries.shape[0]
    seq_count = queries.shape[1]
    positions = lax.axis_index("ep") * pos_count + jnp.arange(pos_count, dtype=jnp.int32)
    q_rot = prepare(queries, positions, query_gain)
    k_rot = prepare(keys, positions, key_gain)
    kv_local = k_rot.shape[2]
    groups = q_rot.shape[2] // kv_local
    value_heads = values.reshape(pos_count, seq_count, kv_local, HEAD_DIM)
    q_group = q_rot.reshape(pos_count, seq_count, kv_local, groups, HEAD_DIM)
    scale = HEAD_DIM ** (-0.5)
    tok_count = moe_tokens.shape[0]
    top_count = routes.shape[1]
    experts = lax.axis_size("ep")
    capacity = max(2, (3 * tok_count * top_count + 2 * experts - 1) // (2 * experts))
    token_float = moe_tokens.astype(jnp.float32)
    normed = (
        token_float
        * lax.rsqrt(jnp.mean(token_float * token_float, axis=-1, keepdims=True) + EPS)
        * moe_gain
    ).astype(jnp.bfloat16)
    hits = (routes[:, :, None] == jnp.arange(experts, dtype=jnp.int32)[None, None, :]).astype(
        jnp.float32
    )
    pair_count = tok_count * top_count
    flat_hits = hits.reshape(pair_count, experts)
    pair_index = jnp.arange(pair_count, dtype=jnp.int32)
    earlier = (pair_index[:, None] > pair_index[None, :]).astype(jnp.float32)
    before = jnp.dot(earlier, flat_hits, precision=lax.Precision.HIGHEST)
    rank = jnp.sum(before * flat_hits, axis=-1).astype(jnp.int32).reshape(tok_count, top_count)
    slot = routes * capacity + rank
    table = jnp.arange(experts * capacity, dtype=jnp.int32)
    dispatch = jnp.sum(
        (slot[None, :, :] == table[:, None, None]).astype(jnp.float32), axis=2
    ).astype(jnp.bfloat16)
    send = jnp.dot(dispatch, normed, preferred_element_type=jnp.float32).astype(jnp.bfloat16)
    kv = jnp.concatenate([k_rot, value_heads], axis=-1)
    kv = jnp.transpose(kv, (1, 2, 0, 3)).reshape(seq_count * kv_local, pos_count, 2 * HEAD_DIM)
    q_rows = jnp.transpose(q_group * jnp.bfloat16(scale), (1, 2, 3, 0, 4))
    q_rows = jnp.pad(q_rows, ((0, 0),) * 4 + ((0, HEAD_DIM),))
    q_rows = q_rows.reshape(seq_count * kv_local, groups * pos_count, 2 * HEAD_DIM)
    returned_rows, attended = fused(
        experts,
        send.reshape(experts, capacity, -1),
        kv,
        q_rows,
        out_weight,
        w_gate[0],
        w_up[0],
        w_down[0],
    )
    returned_rows = returned_rows.reshape(experts * capacity, -1)
    quarter = pos_count // lax.axis_size("tp")
    attended = jnp.transpose(attended.reshape(seq_count, quarter, -1), (1, 0, 2))
    combined = jnp.zeros((tok_count, returned_rows.shape[-1]), jnp.float32)
    for choice_index in range(top_count):
        picker = (slot[:, choice_index : choice_index + 1] == table[None, :]).astype(jnp.bfloat16)
        picked = jnp.dot(picker, returned_rows, preferred_element_type=jnp.float32)
        combined = combined + picked * route_weight[:, choice_index : choice_index + 1]
    return (attended, combined.astype(jnp.bfloat16))


def solution(mesh):
    in_specs = (
        P("ep", None, "tp"),
        P("ep", None, "tp"),
        P("ep", None, "tp"),
        P(),
        P(),
        P("tp", None),
        P(("ep", "tp"), None),
        P(),
        P(("ep", "tp"), None),
        P(("ep", "tp"), None),
        P("ep", None, "tp"),
        P("ep", None, "tp"),
        P("ep", "tp", None),
    )
    out_specs = (P(("ep", "tp"), None, None), P(("ep", "tp"), None))
    return jax.shard_map(
        per_device, mesh=mesh, in_specs=in_specs, out_specs=out_specs, check_vma=False
    )
```

```python
import functools

import jax
import jax.numpy as jnp
from jax import lax
from jax.experimental import pallas as pl
from jax.experimental.pallas import tpu as pltpu
from jax.sharding import PartitionSpec as P

HEAD_DIM = 64
GRID_W = 64


EPS = 1e-06
THETA = 10000.0


def turn(normed, positions):
    quarter = normed.shape[-1] // 4
    inverse = THETA ** (-jnp.arange(quarter, dtype=jnp.float32) / quarter)
    grid_row = (positions // GRID_W).astype(jnp.float32)
    grid_col = (positions % GRID_W).astype(jnp.float32)
    angles = jnp.stack([grid_row[:, None] * inverse, grid_col[:, None] * inverse], axis=1)
    cosine = jnp.cos(angles)[:, None, None]
    sine = jnp.sin(angles)[:, None, None]
    parts = normed.reshape(normed.shape[:-1] + (2, 2, quarter))
    first = parts[..., 0, :]
    second = parts[..., 1, :]
    turned = jnp.stack([first * cosine - second * sine, second * cosine + first * sine], axis=-2)
    return turned.reshape(normed.shape)


def prepare(data, positions, gain):
    heads = data.astype(jnp.float32).reshape(data.shape[0], data.shape[1], -1, HEAD_DIM)
    normed = heads * lax.rsqrt(jnp.mean(heads * heads, axis=-1, keepdims=True) + EPS) * gain
    return turn(normed, positions).astype(jnp.bfloat16)


MESH = pl.DeviceIdType.MESH


def fused_kernel(experts, send, kv, q, out_weight, w_gate, w_up, w_down, ret, att, *scratch):
    (rows, kv_all, part, pair, gone, seen, done, prod, pair_att, gone_att, seen_att, packed, accum, best, total) = scratch[:15]
    (a_send, a_recv, y_send, y_recv, l_send, l_recv, m_send, m_recv, k_send, k_recv, x_send, x_recv) = scratch[15:27]
    (f_send, f_recv, n_send, n_recv, c_send, c_recv, b_send, b_recv, o_send, o_recv, own) = scratch[27:]
    f32, bf16 = jnp.float32, jnp.bfloat16
    e, t = lax.axis_index("ep"), lax.axis_index("tp")
    low, high = t + 1 - 2 * (t % 2), (t + 2) % 4
    low_high = (low + 2) % 4
    half = experts // 2
    side = e + 1 - 2 * (e % 2)
    capacity = send.shape[1]
    stride = packed.shape[0] // 4

    def remote(src, dst, s, r, device):
        return pltpu.make_async_remote_copy(
            src_ref=src, dst_ref=dst, send_sem=s, recv_sem=r, device_id=device, device_id_type=MESH
        )

    def source(k):
        return (e - k + experts) % experts

    def kv_direct(k):
        return remote(kv, kv_all.at[e], k_send.at[k], k_recv.at[k], ((e + 2 * k) % experts, t))

    def kv_side(k):
        block = kv_all.at[(e - 2 * k + experts) % experts]
        return remote(block, block, x_send.at[k], x_recv.at[k], (side, t))

    def chunk(k):
        return remote(send.at[(e + k) % experts], rows.at[t, e], a_send.at[k], a_recv.at[k], ((e + k) % experts, t))

    def across(k):
        block = rows.at[t, source(k)]
        return remote(block, block, y_send.at[k], y_recv.at[k], (e, high))

    def beside(k):
        block = rows.at[t, source(k)]
        return remote(block, block, l_send.at[k], l_recv.at[k], (e, low))

    def relay(k):
        block = rows.at[high, source(k)]
        return remote(block, block, m_send.at[k], m_recv.at[k], (e, low))

    def pair_far(k):
        return remote(part.at[low_high, k], pair.at[1, k], f_send.at[k], f_recv.at[k], (e, low))

    def pair_near(k):
        return remote(part.at[low, k], pair.at[0, k], n_send.at[k], n_recv.at[k], (e, low))

    def over(k):
        return remote(gone.at[k], seen.at[k], c_send.at[k], c_recv.at[k], (e, high))

    def back(k):
        return remote(done.at[k], ret.at[e], b_send.at[k], b_recv.at[k], (source(k), t))

    def other(i):
        if i < 2:
            return remote(prod.at[(low, low_high)[i]], pair_att.at[i], o_send.at[i], o_recv.at[i], (e, low))
        return remote(gone_att, seen_att, o_send.at[i], o_recv.at[i], (e, high))

    def attend(owner):
        for s in range(kv.shape[0]):
            block = kv_all[owner, s]
            scores = lax.dot_general(block, q[s], (((1,), (1,)), ((), ())), preferred_element_type=f32)
            old = best[s]
            new = jnp.maximum(old, jnp.max(scores, axis=0, keepdims=True))
            factor = jnp.exp(old - new)
            expo = jnp.exp(scores - new)
            best[s] = new
            total[s] = total[s] * factor + jnp.sum(expo, axis=0, keepdims=True)
            added = lax.dot_general(block, expo.astype(bf16), (((0,), (0,)), ((), ())), preferred_element_type=f32)
            accum[s] = accum[s] * factor + added

    def project():
        positions = kv.shape[1]
        quarter = positions // 4
        for s in range(kv.shape[0]):
            mixed = (accum[s, HEAD_DIM:, :] / total[s]).astype(bf16)
            groups = mixed.shape[1] // positions
            stacked = jnp.concatenate([mixed[:, g * positions : (g + 1) * positions] for g in range(groups)], axis=0)
            product = lax.dot_general(stacked, out_weight[...], (((0,), (0,)), ((), ())), preferred_element_type=f32)
            product = product.astype(bf16)
            for b in range(4):
                prod[b, s * quarter : (s + 1) * quarter, :] = product[b * quarter : (b + 1) * quarter]

    def expert(k):
        for b in range(4):
            packed[b * stride : b * stride + capacity, :] = rows[b, source(k)]
        data = packed[...]
        gate = jnp.dot(data, w_gate[...], preferred_element_type=f32)
        up = jnp.dot(data, w_up[...], preferred_element_type=f32)
        hidden = (gate * (1.0 / (1.0 + jnp.exp(-gate))) * up).astype(bf16)
        result = jnp.dot(hidden, w_down[...], preferred_element_type=f32).astype(bf16)
        for b in range(4):
            part[b, k] = result[b * stride : b * stride + capacity]

    barrier = pltpu.get_barrier_semaphore()
    partners = [((e + k) % experts, t) for k in range(1, experts)] + [(e, low), (e, high)]
    for device in partners:
        pl.semaphore_signal(barrier, inc=1, device_id=device, device_id_type=MESH)
    pl.semaphore_wait(barrier, len(partners))

    own_chunk = pltpu.make_async_copy(send.at[e], rows.at[t, e], own.at[0])
    own_chunk.start()
    own_kv = pltpu.make_async_copy(kv, kv_all.at[e], own.at[1])
    own_kv.start()
    lax.fori_loop(1, experts, lambda k, c: (chunk(k).start(), c)[1], 0)
    lax.fori_loop(1, half, lambda k, c: (kv_direct(k).start(), c)[1], 0)
    best[...] = jnp.full_like(best, -1e30)
    total[...] = jnp.zeros_like(total)
    accum[...] = jnp.zeros_like(accum)
    own_chunk.wait()
    own_kv.wait()
    kv_side(0).start()

    def step(k, carry):
        @pl.when((k >= 1) & (k < experts))
        def _():
            chunk(k).wait_recv()

        @pl.when(k < experts)
        def _():
            across(k).start()
            beside(k).start()

        @pl.when((k >= 2) & (k < experts + 2))
        def _():
            across(k - 2).wait_recv()
            relay(k - 2).start()

        @pl.when((k >= 4) & (k < experts + 4))
        def _():
            pair_far(k - 4).start()
            pair_near(k - 4).start()

        @pl.when((k >= 3) & (k < experts + 3))
        def _():
            beside(k - 3).wait_recv()
            relay(k - 3).wait_recv()
            expert(k - 3)

        @pl.when((k >= 6) & (k < experts + 6))
        def _():
            over(k - 6).start()

        @pl.when((k >= 5) & (k < experts + 5))
        def _():
            j = k - 5
            pair_far(j).wait_recv()
            gone[j] = (part[high, j].astype(f32) + pair[1, j].astype(f32)).astype(bf16)

        @pl.when(k == experts + 7)
        def _():
            other(1).wait_recv()
            gone_att[...] = (prod[high].astype(f32) + pair_att[1].astype(f32)).astype(bf16)

        @pl.when(k == experts + 9)
        def _():
            other(2).start()

        @pl.when(k == 10)
        def _():
            pltpu.make_async_copy(done.at[0], ret.at[e], own.at[0]).start()

        @pl.when((k >= 11) & (k < experts + 10))
        def _():
            back(k - 10).start()

        @pl.when((k >= 9) & (k < experts + 9))
        def _():
            j = k - 9
            pair_near(j).wait_recv()
            over(j).wait_recv()
            done[j] = (part[t, j].astype(f32) + pair[0, j].astype(f32) + seen[j].astype(f32)).astype(bf16)

        @pl.when((k >= 6) & (k < half + 5))
        def _():
            kv_direct(k - 5).wait_recv()
            kv_side(k - 5).start()

        @pl.when((k >= half + 5) & (k < experts + 5))
        def _():
            kv_side(k - 5 - half).wait_recv()

        @pl.when((k >= 5) & (k < experts + 5))
        def _():
            i = k - 5
            direct = (e - 2 * i + 2 * experts) % experts
            beyond = (side - 2 * (i - half) + 2 * experts) % experts
            near = (experts + half - 1 - i) // experts
            attend(near * direct + (1 - near) * beyond)

        @pl.when(k == experts + 5)
        def _():
            project()

        @pl.when(k == experts + 6)
        def _():
            other(1).start()
            other(0).start()

        return carry

    lax.fori_loop(0, experts + 10, step, 0)
    other(0).wait_recv()
    other(2).wait_recv()
    att[...] = (prod[t].astype(f32) + pair_att[0].astype(f32) + seen_att[...].astype(f32)).astype(bf16)

    def finish(k, carry):
        across(k).wait_send()
        beside(k).wait_send()
        relay(k).wait_send()
        pair_far(k).wait_send()
        pair_near(k).wait_send()
        over(k).wait_send()

        @pl.when(k >= 1)
        def _():
            chunk(k).wait_send()
            back(k).wait()

        @pl.when(k < half)
        def _():
            kv_side(k).wait_send()

        @pl.when((k >= 1) & (k < half))
        def _():
            kv_direct(k).wait_send()

        return carry

    lax.fori_loop(0, experts, finish, 0)
    for i in range(3):
        other(i).wait_send()
    pltpu.make_async_copy(done.at[0], ret.at[e], own.at[0]).wait()


def fused(experts, send, kv, q, out_weight, w_gate, w_up, w_down):
    sem = pltpu.SemaphoreType.DMA((experts,))
    like = send.dtype
    capacity, features = send.shape[1:]
    seqs, positions, lanes = kv.shape
    att = (positions // 4 * seqs, features)
    queries = q.shape[1]
    stride = -(-capacity // 16) * 16
    shapes = [
        (4,) + send.shape,
        (experts,) + kv.shape,
        (4,) + send.shape,
        (2,) + send.shape,
        send.shape,
        send.shape,
        send.shape,
        (4,) + att,
        (2,) + att,
        att,
        att,
        (4 * stride, features),
    ]
    vmem = pl.BlockSpec(memory_space=pltpu.VMEM)
    return pl.pallas_call(
        functools.partial(fused_kernel, experts),
        out_shape=(jax.ShapeDtypeStruct(send.shape, like), jax.ShapeDtypeStruct(att, like)),
        in_specs=[vmem] * 7,
        out_specs=(vmem, vmem),
        scratch_shapes=[pltpu.VMEM(shape, like) for shape in shapes]
        + [
            pltpu.VMEM((seqs, lanes, queries), jnp.float32),
            pltpu.VMEM((seqs, 1, queries), jnp.float32),
            pltpu.VMEM((seqs, 1, queries), jnp.float32),
        ]
        + [sem] * 20
        + [pltpu.SemaphoreType.DMA((3,))] * 2
        + [pltpu.SemaphoreType.DMA((2,))],
        name="fused",
        compiler_params=pltpu.CompilerParams(
            collective_id=1, has_side_effects=True, vmem_limit_bytes=62 * 2**20
        ),
    )(send, kv, q, out_weight, w_gate, w_up, w_down)


def per_device(
    queries,
    keys,
    values,
    query_gain,
    key_gain,
    out_weight,
    moe_tokens,
    moe_gain,
    routes,
    route_weight,
    w_gate,
    w_up,
    w_down,
):
    pos_count = queries.shape[0]
    seq_count = queries.shape[1]
    positions = lax.axis_index("ep") * pos_count + jnp.arange(pos_count, dtype=jnp.int32)
    q_rot = prepare(queries, positions, query_gain)
    k_rot = prepare(keys, positions, key_gain)
    kv_local = k_rot.shape[2]
    groups = q_rot.shape[2] // kv_local
    value_heads = values.reshape(pos_count, seq_count, kv_local, HEAD_DIM)
    q_group = q_rot.reshape(pos_count, seq_count, kv_local, groups, HEAD_DIM)
    scale = HEAD_DIM ** (-0.5)
    tok_count = moe_tokens.shape[0]
    top_count = routes.shape[1]
    experts = lax.axis_size("ep")
    capacity = max(2, (3 * tok_count * top_count + 2 * experts - 1) // (2 * experts))
    token_float = moe_tokens.astype(jnp.float32)
    normed = (
        token_float
        * lax.rsqrt(jnp.mean(token_float * token_float, axis=-1, keepdims=True) + EPS)
        * moe_gain
    ).astype(jnp.bfloat16)
    hits = (routes[:, :, None] == jnp.arange(experts, dtype=jnp.int32)[None, None, :]).astype(
        jnp.float32
    )
    pair_count = tok_count * top_count
    flat_hits = hits.reshape(pair_count, experts)
    pair_index = jnp.arange(pair_count, dtype=jnp.int32)
    earlier = (pair_index[:, None] > pair_index[None, :]).astype(jnp.float32)
    before = jnp.dot(earlier, flat_hits, precision=lax.Precision.HIGHEST)
    rank = jnp.sum(before * flat_hits, axis=-1).astype(jnp.int32).reshape(tok_count, top_count)
    slot = routes * capacity + rank
    table = jnp.arange(experts * capacity, dtype=jnp.int32)
    dispatch = jnp.sum(
        (slot[None, :, :] == table[:, None, None]).astype(jnp.float32), axis=2
    ).astype(jnp.bfloat16)
    send = jnp.dot(dispatch, normed, preferred_element_type=jnp.float32).astype(jnp.bfloat16)
    kv = jnp.concatenate([k_rot, value_heads], axis=-1)
    kv = jnp.transpose(kv, (1, 2, 0, 3)).reshape(seq_count * kv_local, pos_count, 2 * HEAD_DIM)
    q_rows = jnp.transpose(q_group * jnp.bfloat16(scale), (1, 2, 3, 0, 4))
    q_rows = jnp.pad(q_rows, ((0, 0),) * 4 + ((0, HEAD_DIM),))
    q_rows = q_rows.reshape(seq_count * kv_local, groups * pos_count, 2 * HEAD_DIM)
    returned_rows, attended = fused(
        experts,
        send.reshape(experts, capacity, -1),
        kv,
        q_rows,
        out_weight,
        w_gate[0],
        w_up[0],
        w_down[0],
    )
    returned_rows = returned_rows.reshape(experts * capacity, -1)
    quarter = pos_count // lax.axis_size("tp")
    attended = jnp.transpose(attended.reshape(seq_count, quarter, -1), (1, 0, 2))
    combined = jnp.zeros((tok_count, returned_rows.shape[-1]), jnp.float32)
    for choice_index in range(top_count):
        picker = (slot[:, choice_index : choice_index + 1] == table[None, :]).astype(jnp.bfloat16)
        picked = jnp.dot(picker, returned_rows, preferred_element_type=jnp.float32)
        combined = combined + picked * route_weight[:, choice_index : choice_index + 1]
    return (attended, combined.astype(jnp.bfloat16))


def solution(mesh):
    in_specs = (
        P("ep", None, "tp"),
        P("ep", None, "tp"),
        P("ep", None, "tp"),
        P(),
        P(),
        P("tp", None),
        P(("ep", "tp"), None),
        P(),
        P(("ep", "tp"), None),
        P(("ep", "tp"), None),
        P("ep", None, "tp"),
        P("ep", None, "tp"),
        P("ep", "tp", None),
    )
    out_specs = (P(("ep", "tp"), None, None), P(("ep", "tp"), None))
    return jax.shard_map(
        per_device, mesh=mesh, in_specs=in_specs, out_specs=out_specs, check_vma=False
    )
```
